512 devices in a mesh: ep: 128 (over z, y, core), tp: 4 (over x).
Axes of the slice: x: 4, y: 8, z: 8, core: 2. Of those that a mesh axis runs over, the one named last changes fastest.
Arguments:
- tokens: bfloat16 [8192, 1024], P('ep', 'tp'), may hold values from -6 to 6
- conv_state: bfloat16 [8192, 3, 512], P('ep', None, 'tp'), may hold values from -6 to 6
- lru_state: float32 [8192, 512], P('ep', 'tp'), may hold values from -6 to 6
- mix_gain: bfloat16 [1024], replicated, may hold values from 0.099609375 to 1.8984375
- ffn_gain: bfloat16 [1024], replicated, may hold values from 0.099609375 to 1.8984375
- w_branch: bfloat16 [1024, 512], P(None, 'tp'), may hold values from -0.1875 to 0.1875
- w_gate: bfloat16 [1024, 512], P(None, 'tp'), may hold values from -0.1875 to 0.1875
- conv_taps: bfloat16 [4, 512], P(None, 'tp'), may hold values from -3 to 3
- w_recur: bfloat16 [8, 64, 64], P('tp'), may hold values from -0.75 to 0.75
- w_inject: bfloat16 [8, 64, 64], P('tp'), may hold values from -0.75 to 0.75
- lru_lambda: float32 [512], P('tp'), may hold values from 2 to 7
- w_out: bfloat16 [512, 1024], P('tp'), may hold values from -0.25 to 0.25
- expert_gate: bfloat16 [128, 1024, 2560], P('ep', None, 'tp'), may hold values from -0.1875 to 0.1875
- expert_up: bfloat16 [128, 1024, 2560], P('ep', None, 'tp'), may hold values from -0.1875 to 0.1875
- expert_down: bfloat16 [128, 2560, 1024], P('ep', 'tp'), may hold values from -0.125 to 0.125
- route_ids: int32 [8192, 2], P('ep'), may hold values from 0 to 127, all different within a row; in each aligned block of 64 rows (0 to 63, 64 to 127, ...) at most 2 rows name the same one
- route_weight: float32 [8192, 2], P('ep'), may hold values from 0.2 to 1
Outputs:
- mixed: bfloat16 [8192, 1024], P('ep', 'tp')
- state_out: float32 [8192, 512], P('ep', 'tp')
The draws below stay inside these ranges and needn't reach their ends.
Inputs may be any that keep to these rules, and one draw needn't show every extreme that they name: `route_ids`: each row names 2 different experts. Among the 64 rows of one device no expert is named more than 2 times, and in every draw some expert is named exactly 2 times by them.
All inputs are finite; a program needn't handle non-finite values.
Results may differ from the reference program's by a relative error of at most 0.015.
Values may be sent and summed in bfloat16 or wider, within the bound.
A program may use at most 64 MiB of HBM per device.

```python
import math
import jax
import jax.numpy as jnp
import numpy as np
from jax import lax

D = 1024
HEADS = 8
HEAD_W = 64
W_A = 512
CONV = 4
FF = 2560
SEQS = 64
TOP = 2
EXPERTS = 128
CAP = 2
SEQ_ALL = 8192
N_TP = 4


def block_levels(stream_key, dims, shards, smallest, largest):
    loudness = 1.0
    for axis_at, shards_of in shards:
        heights = jax.random.uniform(jax.random.fold_in(jax.random.fold_in(stream_key, 6), axis_at), (shards_of,), jnp.float32, smallest / len(shards), largest / len(shards))
        loudness = loudness * jnp.repeat(jnp.exp(heights), dims[axis_at] // shards_of).reshape((-1,) + (1,) * (len(dims) - 1 - axis_at))
    return loudness


def routed_block(rng, own, number, rows, number_of, top, reach, skew):
    ranking = jax.random.permutation(rng, number_of)
    packed, usual = shares(number_of, rows * top, reach, skew, True), shares(number_of, rows * top, reach, skew, False)
    places = jnp.arange(number_of)

    def named(tallies, rotation):
        used = int((tallies > 0).sum())
        fixed = max(1, used // 4)
        moved = fixed + (places - fixed + rotation * (used - fixed)) % max(1, number_of - fixed)
        return jnp.zeros((number_of,), jnp.int32).at[ranking[jnp.where(places < fixed, places, moved)]].set(jnp.asarray(tallies, jnp.int32))

    tallies = jnp.where(number % 4 == 0, named(packed, number // 4), named(usual, number - number // 4 - 1))
    mixed = jax.random.permutation(jax.random.fold_in(own, 3), number_of)
    donor, sink = mixed[0:number_of // 2 * 2:2], mixed[1:number_of // 2 * 2:2]
    slack = jnp.minimum(tallies[donor] - 1, reach - tallies[sink]) // 2
    slack = jnp.where((donor == ranking[0]) | (sink == ranking[0]) | (tallies[sink] == 0), 0, jnp.maximum(slack, 0))
    moved = jax.random.randint(jax.random.fold_in(own, 4), (number_of // 2,), 0, 1 << 20) % (slack + 1)
    tallies = tallies.at[donor].add(-moved).at[sink].add(moved)
    items = jnp.searchsorted(jnp.cumsum(tallies), jnp.arange(rows * top), side="right").astype(jnp.int32)
    table = items.reshape(top, rows).T
    table = table[jax.random.permutation(jax.random.fold_in(own, 1), rows)]
    rotation = jax.random.randint(jax.random.fold_in(own, 2), (rows, 1), 0, top)
    return jnp.take_along_axis(table, (jnp.arange(top)[None, :] + rotation) % top, axis=1)


def shares(count, total, reach, skew, full):
    loads = [(1 << 20) // math.isqrt(grade ** skew) + 1 for grade in range(1, count + 1)]
    largest = reach if full else min(reach, max(-(-total // count), total * loads[0] // sum(loads)))
    least = 1 if total - largest >= count - 1 else 0
    given, surplus = [largest] + [least] * (count - 1), total - largest - least * (count - 1)
    while surplus > 0:
        candidates = [i for i in range(1, count) if given[i] < largest] or [i for i in range(1, count) if given[i] < reach]
        whole, remaining = sum([loads[i] for i in candidates]), surplus
        for i in candidates:
            extra = min(reach - given[i], max(1, remaining * loads[i] // whole), surplus)
            given[i] = given[i] + extra
            surplus = surplus - extra
    return np.array(given)


def gaussian(stream_key, dims, spread, limit, pieces=(), kind=jnp.bfloat16):
    factor_of = block_levels(stream_key, dims, pieces, -0.22, 0.18) if pieces else 1.0
    result = jax.random.normal(stream_key, dims, jnp.float32) * spread * factor_of
    return jnp.minimum(jnp.maximum(result, -limit), limit).astype(kind)


def setup_inputs(seed: int = 0) -> dict:
    splits = jax.random.split(jax.random.key(seed), 18)
    tokens = gaussian(splits[0], (SEQ_ALL, D), 1.0, 6.0, ((0, 128), (1, 4)))
    conv_state = gaussian(splits[1], (SEQ_ALL, CONV - 1, W_A), 1.0, 6.0, ((0, 128), (2, 4)))
    lru_state = gaussian(splits[2], (SEQ_ALL, W_A), 1.0, 6.0, ((0, 128), (1, 4)), jnp.float32)
    mix_gain = jnp.clip(1.0 + 0.18 * jax.random.normal(splits[3], (D,), jnp.float32), 0.099609375, 1.8984375).astype(jnp.bfloat16)
    ffn_gain = jnp.clip(1.0 + 0.18 * jax.random.normal(splits[4], (D,), jnp.float32), 0.099609375, 1.8984375).astype(jnp.bfloat16)
    w_branch = gaussian(splits[5], (D, W_A), D ** -0.5, 0.1875, ((1, 4),))
    w_gate = gaussian(splits[6], (D, W_A), D ** -0.5, 0.1875, ((1, 4),))
    conv_taps = gaussian(splits[7], (CONV, W_A), 0.5, 3.0, ((1, 4),))
    w_recur = gaussian(splits[8], (HEADS, HEAD_W, HEAD_W), HEAD_W ** -0.5, 0.75, ((0, 4),))
    w_inject = gaussian(splits[9], (HEADS, HEAD_W, HEAD_W), HEAD_W ** -0.5, 0.75, ((0, 4),))
    lru_lambda = jnp.clip(2.0 + 5.0 * jax.random.uniform(splits[10], (W_A,), jnp.float32) ** block_levels(splits[10], (W_A,), ((0, 4),), -0.2, 0.2), 2.0, 7.0)
    w_out = gaussian(splits[11], (W_A, D), W_A ** -0.5, 0.25, ((0, 4),))
    expert_gate = gaussian(splits[12], (EXPERTS, D, FF), D ** -0.5, 0.1875, ((0, 128), (2, 4)))
    expert_up = gaussian(splits[13], (EXPERTS, D, FF), D ** -0.5, 0.1875, ((0, 128), (2, 4)))
    expert_down = gaussian(splits[14], (EXPERTS, FF, D), FF ** -0.5, 0.125, ((0, 128), (1, 4)))
    route_ids_keys = jax.random.split(jax.random.fold_in(splits[15], 1), SEQ_ALL // SEQS)
    route_ids_turns = jax.random.permutation(jax.random.fold_in(splits[15], 3), SEQ_ALL // SEQS)
    route_ids = jax.vmap(lambda own, number: routed_block(jax.random.fold_in(splits[15], 2), own, number, SEQS, EXPERTS, TOP, CAP, 2))(route_ids_keys, route_ids_turns).reshape((SEQ_ALL, TOP))
    route_weight = jnp.clip(0.2 + 0.8 * jax.random.uniform(splits[16], (SEQ_ALL, TOP), jnp.float32) ** block_levels(splits[16], (SEQ_ALL, TOP), ((0, 128),), -0.2, 0.2), 0.2, 1.0)
    return {"tokens": tokens, "conv_state": conv_state, "lru_state": lru_state, "mix_gain": mix_gain, "ffn_gain": ffn_gain, "w_branch": w_branch, "w_gate": w_gate, "conv_taps": conv_taps, "w_recur": w_recur, "w_inject": w_inject, "lru_lambda": lru_lambda, "w_out": w_out, "expert_gate": expert_gate, "expert_up": expert_up, "expert_down": expert_down, "route_ids": route_ids, "route_weight": route_weight}


EPS = 1e-06
LRU_SCALE = 8.0

def rms_rows(rows, gain):
    values = rows.astype(jnp.float32)
    scaled = values * lax.rsqrt(lax.optimization_barrier(jnp.mean(values * values, axis=-1, keepdims=True)) + EPS)
    return (scaled * gain.astype(jnp.float32)).astype(jnp.bfloat16)

def split_sum(left, right, groups):
    count = left.shape[0]
    width = left.shape[1] // groups
    parts = jnp.einsum('ngk,gkm->ngm', left.reshape(count, groups, width).astype(jnp.float32), right.reshape(groups, width, right.shape[1]).astype(jnp.float32))
    rounded = lax.optimization_barrier(parts.astype(jnp.bfloat16)).astype(jnp.float32)
    return lax.optimization_barrier(jnp.sum(rounded, axis=1)).astype(jnp.bfloat16)

def reference(tokens, conv_state, lru_state, mix_gain, ffn_gain, w_branch, w_gate, conv_taps, w_recur, w_inject, lru_lambda, w_out, expert_gate, expert_up, expert_down, route_ids, route_weight):
    count = tokens.shape[0]
    normed = rms_rows(tokens, mix_gain)
    branch = jnp.dot(normed, w_branch, preferred_element_type=jnp.float32).astype(jnp.bfloat16)
    gate_in = jnp.dot(normed, w_gate, preferred_element_type=jnp.float32).astype(jnp.bfloat16)
    window = jnp.concatenate([conv_state, branch[:, None, :]], axis=1).astype(jnp.float32)
    conv_out = lax.optimization_barrier(jnp.sum(window * conv_taps.astype(jnp.float32)[None], axis=1))
    conv_heads = lax.optimization_barrier(conv_out.astype(jnp.bfloat16)).astype(jnp.float32).reshape(count, HEADS, HEAD_W)
    recur = jax.nn.sigmoid(jnp.einsum('nhi,hij->nhj', conv_heads, w_recur.astype(jnp.float32)).reshape(count, HEADS * HEAD_W))
    inject = jax.nn.sigmoid(jnp.einsum('nhi,hij->nhj', conv_heads, w_inject.astype(jnp.float32)).reshape(count, HEADS * HEAD_W))
    log_decay = -LRU_SCALE * recur * jax.nn.softplus(-lru_lambda)
    state_out = jnp.exp(log_decay) * lru_state + jnp.sqrt(-jnp.expm1(2.0 * log_decay)) * inject * conv_out
    lru_out = (state_out * jax.nn.gelu(gate_in.astype(jnp.float32))).astype(jnp.bfloat16)
    mix_out = split_sum(lru_out, w_out, N_TP)
    resid = (tokens.astype(jnp.float32) + mix_out.astype(jnp.float32)).astype(jnp.bfloat16)
    normed2 = rms_rows(resid, ffn_gain)
    groups = count // SEQS
    flat = route_ids.reshape(groups, SEQS * TOP).astype(jnp.int32)
    onehot = (flat[:, :, None] == jnp.arange(EXPERTS, dtype=jnp.int32)[None, None, :]).astype(jnp.int32)
    before = jnp.cumsum(onehot, axis=1) - onehot
    slot = lax.optimization_barrier(jnp.sum(before * onehot, axis=2)).astype(jnp.int32)
    where = (jnp.arange(groups, dtype=jnp.int32)[:, None] * CAP + slot).reshape(-1).astype(jnp.int32)
    token_of = (jnp.arange(groups, dtype=jnp.int32)[:, None] * SEQS + jnp.arange(SEQS * TOP, dtype=jnp.int32)[None, :] // TOP).reshape(-1).astype(jnp.int32)
    expert_of = flat.reshape(-1)
    table = jnp.full((EXPERTS, groups * CAP), count, jnp.int32).at[expert_of, where].set(token_of)
    padded = jnp.concatenate([normed2, jnp.zeros((1, D), jnp.bfloat16)], axis=0)

    def one_expert(args):
        rows_idx, e_gate, e_up, e_down = args
        rows = padded[rows_idx].astype(jnp.float32)
        first = jnp.dot(rows, e_gate.astype(jnp.float32))
        second = jnp.dot(rows, e_up.astype(jnp.float32))
        hidden = (jax.nn.silu(first) * second).astype(jnp.bfloat16)
        return split_sum(hidden, e_down, N_TP)
    outputs = lax.map(one_expert, (table, expert_gate, expert_up, expert_down))
    picked = outputs[expert_of, where].reshape(count, TOP, D).astype(jnp.float32)
    moe = lax.optimization_barrier(jnp.sum(picked * route_weight[:, :, None], axis=1))
    mixed = (resid.astype(jnp.float32) + moe).astype(jnp.bfloat16)
    return (mixed, state_out)
```

```python
import functools

import jax
import jax.numpy as jnp
from jax import lax
from jax.experimental import pallas as pl
from jax.experimental.pallas import tpu as pltpu
from jax.sharding import PartitionSpec as P

EPS = 1e-06
LRU_SCALE = 8.0
MESH = pl.DeviceIdType.MESH
F32 = jnp.float32
BF16 = jnp.bfloat16

NX = 4
NZ = 8
NG = 16
S = 64
CAP = 2
F = 256
H = 128
ROWS = NZ * NG * CAP
D = NX * F
CH = 2
CR = ROWS // CH

RING8 = (4, 3, 5, 2, 6, 1, 7)


def remote(src, dst, send, recv, dev):
    return pltpu.make_async_remote_copy(
        src_ref=src, dst_ref=dst, send_sem=send, recv_sem=recv, device_id=dev, device_id_type=MESH
    )


def iota(shape, dim):
    return lax.broadcasted_iota(jnp.int32, shape, dim)


def dot(a, b):
    return jnp.dot(a, b, preferred_element_type=F32)


def swap_matrix(outer, inner):
    row = iota((ROWS, ROWS), 0)
    col = iota((ROWS, ROWS), 1)
    slot = lax.rem(row, CAP)
    mid = lax.rem(lax.div(row, CAP), inner)
    top = lax.div(row, CAP * inner)
    source = mid * (outer * CAP) + top * CAP + slot
    return jnp.where(col == source, 1.0, 0.0).astype(BF16)


def kernel(
    tokens,
    conv_state,
    lru_state,
    mix_gain,
    ffn_gain,
    w_branch,
    w_gate,
    conv_taps,
    w_recur,
    w_inject,
    lru_lambda,
    w_out,
    expert_gate,
    expert_up,
    expert_down,
    ids,
    weights,
    mixed_out,
    state_out,
    xg,
    conv_v,
    lru_v,
    mixg_v,
    ffng_v,
    wb_v,
    wg_v,
    taps_v,
    wr_v,
    wi_v,
    lam_v,
    wo_v,
    eg_v,
    eu_v,
    ed_v,
    ids_v,
    rw_v,
    bd,
    pick_a,
    pick_b,
    comb_a,
    comb_b,
    to_zg,
    to_gz,
    part,
    mr,
    send_a,
    send_b,
    got_a,
    got_b,
    fwd_a,
    fwd_b,
    all_a,
    all_b,
    xn,
    term_a,
    term_b,
    rel_a,
    rel_b,
    sum_a,
    sum_b,
    rs_a,
    rs_b,
    ret_a,
    ret_b,
    hop_a,
    hop_b,
    mid_a,
    mid_b,
    back_a,
    back_b,
    in_sem,
    tok_s,
    tok_r,
    mix_s,
    mix_r,
    g_s,
    g_r,
    z_s,
    z_r,
    ax_s,
    ax_r,
    bx_s,
    bx_r,
    rs_s,
    rs_r,
):
    x = lax.axis_index("tp")
    e = lax.axis_index("ep")
    z = lax.div(e, NG)
    g = lax.rem(e, NG)
    y = lax.div(g, 2)
    c = lax.rem(g, 2)

    x_dev = [(e, lax.rem(x + d, NX)) for d in range(NX)]
    x_idx = [lax.rem(x + d, NX) for d in range(NX)]
    z_peers = []
    for dz in RING8:
        i = lax.rem(z + dz, NZ)
        z_peers.append((i, (i * NG + g, x)))
    g_peers = []
    for dy in RING8 + (0,):
        for dc in (0, 1):
            if dy or dc:
                i = lax.rem(y + dy, 8) * 2 + lax.rem(c + dc, 2)
                g_peers.append((i, (z * NG + i, x)))

    barrier = pltpu.get_barrier_semaphore()
    for _, dev in z_peers + g_peers:
        pl.semaphore_signal(barrier, inc=1, device_id=dev, device_id_type=MESH)
    for dev in x_dev[1:]:
        pl.semaphore_signal(barrier, inc=1, device_id=dev, device_id_type=MESH)

    loads = {}
    pairs = (
        ("tok", tokens, xg.at[x]),
        ("ids", ids, ids_v),
        ("rw", weights, rw_v),
        ("mixg", mix_gain, mixg_v),
        ("conv", conv_state, conv_v),
        ("taps", conv_taps, taps_v),
        ("wb", w_branch, wb_v),
        ("wg", w_gate, wg_v),
        ("wr", w_recur, wr_v),
        ("wi", w_inject, wi_v),
        ("lam", lru_lambda, lam_v),
        ("lru", lru_state, lru_v),
        ("wo", w_out, wo_v),
        ("ffng", ffn_gain, ffng_v),
        ("eg", expert_gate, eg_v),
        ("eu", expert_up, eu_v),
        ("ed", expert_down, ed_v),
    )
    for i, (name, src, dst) in enumerate(pairs):
        loads[name] = pltpu.make_async_copy(src, dst, in_sem.at[i])
        loads[name].start()

    loads["tok"].wait()
    pl.semaphore_wait(barrier, len(z_peers) + len(g_peers) + NX - 1)

    sends = []

    def start(copy):
        copy.start()
        sends.append(copy)

    for d in (2, 1, 3):
        start(remote(xg.at[x], xg.at[x], tok_s.at[d], tok_r.at[x], x_dev[d]))

    loads["ids"].wait()
    loads["rw"].wait()
    for pick, comb, outer, inner in ((pick_a, comb_a, NG, NZ), (pick_b, comb_b, NZ, NG)):
        row = iota((ROWS, S), 0)
        slot = lax.rem(row, CAP).astype(F32)
        first = lax.rem(lax.div(row, CAP), inner)
        second = lax.div(row, CAP * inner)
        expert = first * NG + second if outer == NG else second * NG + first
        hit0 = jnp.where(ids_v[0:1, :] == expert, 1.0, 0.0)
        hit1 = jnp.where(ids_v[1:2, :] == expert, 1.0, 0.0)
        hit = hit0 + hit1
        earlier = jnp.where(iota((S, S), 0) < iota((S, S), 1), 1.0, 0.0).astype(BF16)
        before = dot(hit.astype(BF16), earlier)
        chosen = jnp.where(before == slot, hit, 0.0)
        pick[...] = chosen.astype(BF16)
        weight = jnp.where(before == slot, hit0 * rw_v[0:1, :] + hit1 * rw_v[1:2, :], 0.0)
        weight = jnp.transpose(weight)
        high = weight.astype(BF16)
        comb[:, 0:ROWS] = high
        comb[:, ROWS:] = (weight - high.astype(F32)).astype(BF16)
    to_zg[...] = swap_matrix(NZ, NG)
    to_gz[...] = swap_matrix(NG, NZ)

    loads["wr"].wait()
    loads["wi"].wait()
    bd[...] = jnp.zeros_like(bd)
    for h in range(2):
        lo, hi = 64 * h, 64 * h + 64
        for k, w in enumerate((wr_v, wi_v)):
            bd[lo:hi, H * k + lo : H * k + hi] = w[h]
    loads["conv"].wait()
    loads["taps"].wait()
    taps = taps_v[...].astype(F32)
    old = (
        conv_v[0].astype(F32) * taps[0:1]
        + conv_v[1].astype(F32) * taps[1:2]
        + conv_v[2].astype(F32) * taps[2:3]
    )
    loads["lam"].wait()
    decay = -LRU_SCALE * jax.nn.softplus(-lam_v[...])
    loads["lru"].wait()
    loads["mixg"].wait()
    gain = mixg_v[...].astype(F32)
    for name in ("wb", "wg", "wo"):
        loads[name].wait()

    for d in (1, 3, 2):
        remote(xg.at[x], xg.at[x_idx[d]], tok_s.at[d], tok_r.at[x_idx[d]], x_dev[d]).wait_recv()
    whole = jnp.concatenate([xg[k].astype(F32) for k in range(NX)], axis=1)
    scale = lax.rsqrt(jnp.sum(whole * whole, axis=1, keepdims=True) * (1.0 / D) + EPS)
    normed = (whole * scale * gain).astype(BF16)
    branch = dot(normed, wb_v[...]).astype(BF16)
    gate_in = dot(normed, wg_v[...]).astype(BF16).astype(F32)
    conv_out = old + branch.astype(F32) * taps[3:4]
    gates = jax.nn.sigmoid(dot(conv_out.astype(BF16), bd[...]))
    recur, inject = gates[:, :H], gates[:, H:]
    log_decay = recur * decay
    state = (
        jnp.exp(log_decay) * lru_v[...]
        + jnp.sqrt(1.0 - jnp.exp(2.0 * log_decay)) * inject * conv_out
    )
    state_out[...] = state
    lru_out = (state * jax.nn.gelu(gate_in)).astype(BF16)
    partial = dot(lru_out, wo_v[...]).astype(BF16)
    for k in range(NX):
        part[k] = partial[:, F * k : F * k + F]
    for d in (2, 1, 3):
        start(remote(part.at[x_idx[d]], mr.at[x], mix_s.at[d], mix_r.at[x], x_dev[d]))
    mix = part[x].astype(F32)
    for d in (1, 3, 2):
        remote(part.at[x], mr.at[x_idx[d]], mix_s.at[d], mix_r.at[x_idx[d]], x_dev[d]).wait_recv()
        mix = mix + mr[x_idx[d]].astype(F32)
    resid = (xg[x].astype(F32) + mix.astype(BF16).astype(F32)).astype(BF16)

    def exchange(way, peers, own, src, dst, s, r):
        for i, (p, dev) in enumerate(peers):
            start(remote(src.at[p], dst.at[own], s.at[way, i], r.at[way, own], dev))

    def arrived(way, i, p, dev, src, dst, s, r):
        remote(src.at[p], dst.at[p], s.at[way, i], r.at[way, p], dev).wait_recv()

    def all_arrived(way, peers, src, dst, s, r):
        for i, (p, dev) in reversed(list(enumerate(peers))):
            arrived(way, i, p, dev, src, dst, s, r)

    send_a[...] = dot(pick_a[...], resid[:, :H]).astype(BF16).reshape(NG, NZ * CAP, H)
    exchange(0, g_peers, g, send_a, got_a, g_s, g_r)
    send_b[...] = dot(pick_b[...], resid[:, H:]).astype(BF16).reshape(NZ, NG * CAP, H)
    exchange(0, z_peers, z, send_b, got_b, z_s, z_r)
    got_a[g] = send_a[g]
    got_b[z] = send_b[z]
    all_arrived(0, z_peers, send_b, got_b, z_s, z_r)
    fwd_b[...] = dot(to_gz[...], got_b[...].reshape(ROWS, H)).astype(BF16).reshape(NG, NZ * CAP, H)
    exchange(1, g_peers, g, fwd_b, all_b.at[x], g_s, g_r)
    all_arrived(0, g_peers, send_a, got_a, g_s, g_r)
    fwd_a[...] = dot(to_zg[...], got_a[...].reshape(ROWS, H)).astype(BF16).reshape(NZ, NG * CAP, H)
    exchange(1, z_peers, z, fwd_a, all_a.at[x], z_s, z_r)
    all_a[x, z] = fwd_a[z]
    all_b[x, g] = fwd_b[g]

    steps = (0, 1, 7, 2, 6, 3, 5, 4)
    left, right = x_idx[3], x_idx[1]

    def pass_on(j, a_src, a_to, b_src, b_to, lane):
        dz = lax.rem(z + steps[j], NZ)
        dy = lax.rem(y + steps[j], 8) * 2
        a = all_a.at[a_src, dz]
        b = all_b.at[b_src, pl.ds(dy, 2)]
        start(remote(a, a, ax_s.at[lane, j], ax_r.at[a_src, j], x_dev[a_to]))
        start(remote(b, b, bx_s.at[lane, j], bx_r.at[b_src, j], x_dev[b_to]))

    def took(src, j, a_too=True, b_too=True):
        dz = lax.rem(z + steps[j], NZ)
        dy = lax.rem(y + steps[j], 8) * 2
        if a_too:
            a = all_a.at[src, dz]
            remote(a, a, ax_s.at[0, j], ax_r.at[src, j], x_dev[1]).wait_recv()
        if b_too:
            b = all_b.at[src, pl.ds(dy, 2)]
            remote(b, b, bx_s.at[0, j], bx_r.at[src, j], x_dev[1]).wait_recv()

    def relay(j):
        took(left, j, b_too=False)
        took(right, j, a_too=False)
        pass_on(j, left, 1, right, 3, 2)

    lag = 3
    for j in range(NZ):
        if steps[j]:
            i = RING8.index(steps[j])
            p, dev = z_peers[i]
            arrived(1, i, p, dev, fwd_a, all_a.at[x], z_s, z_r)
            for i in (2 * i, 2 * i + 1):
                p, dev = g_peers[i]
                arrived(1, i, p, dev, fwd_b, all_b.at[x], g_s, g_r)
        else:
            p, dev = g_peers[14]
            arrived(1, 14, p, dev, fwd_b, all_b.at[x], g_s, g_r)
        pass_on(j, x, 1, x, 1, 0)
        pass_on(j, x, 3, x, 3, 1)
        if j >= lag:
            relay(j - lag)
    for j in range(NZ - lag, NZ):
        relay(j)
    for j in range(NZ):
        took(left, j, a_too=False)
        took(right, j, b_too=False)
    for j in range(NZ):
        took(x_idx[2], j)

    loads["ffng"].wait()
    full_b = jnp.concatenate([all_b[k].reshape(ROWS, H) for k in range(NX)], axis=1)
    full_b = dot(to_zg[...], full_b)
    pieces = []
    for k in range(NX):
        pieces.append(all_a[k].reshape(ROWS, H).astype(F32))
        pieces.append(full_b[:, H * k : H * k + H])
    rows = jnp.concatenate(pieces, axis=1)
    scale = lax.rsqrt(jnp.sum(rows * rows, axis=1, keepdims=True) * (1.0 / D) + EPS)
    xn[...] = (rows * scale * ffng_v[...].astype(F32)).astype(BF16)

    for name in ("eg", "eu", "ed"):
        loads[name].wait()

    def expert(j):
        at = slice(CR * j, CR * j + CR)
        rows = xn[at, :]
        first = dot(rows, eg_v[0])
        second = dot(rows, eu_v[0])
        hidden = (first * jax.nn.sigmoid(first) * second).astype(BF16)
        term = dot(hidden, ed_v[0]).astype(BF16)
        for k in range(NX):
            term_a[j, k] = term[:, F * k : F * k + H]
            term_b[j, k] = term[:, F * k + H : F * k + F]
        start(remote(term_a.at[j, x_idx[2]], rel_a.at[j], rs_s.at[j, 0], rs_r.at[j, 0], x_dev[1]))
        start(remote(term_b.at[j, x_idx[2]], rel_b.at[j], rs_s.at[j, 1], rs_r.at[j, 1], x_dev[3]))
        start(remote(term_b.at[j, right], rs_b.at[j, 0], rs_s.at[j, 2], rs_r.at[j, 2], x_dev[1]))
        start(remote(term_a.at[j, left], rs_a.at[j, 0], rs_s.at[j, 3], rs_r.at[j, 3], x_dev[3]))

    def landed(dst, j, lane):
        remote(dst, dst, rs_s.at[j, lane], rs_r.at[j, lane], x_dev[1]).wait_recv()

    def halfway(j):
        landed(rel_a.at[j], j, 0)
        sum_a[j] = (term_a[j, right].astype(F32) + rel_a[j].astype(F32)).astype(BF16)
        start(remote(sum_a.at[j], rs_a.at[j, 1], rs_s.at[j, 4], rs_r.at[j, 4], x_dev[1]))
        landed(rel_b.at[j], j, 1)
        sum_b[j] = (term_b[j, left].astype(F32) + rel_b[j].astype(F32)).astype(BF16)
        start(remote(sum_b.at[j], rs_b.at[j, 1], rs_s.at[j, 5], rs_r.at[j, 5], x_dev[3]))

    expert(0)
    expert(1)
    halfway(0)
    halfway(1)
    total_b = []
    for j in range(CH):
        landed(rs_a.at[j, 0], j, 3)
        landed(rs_b.at[j, 0], j, 2)
        landed(rs_a.at[j, 1], j, 4)
        landed(rs_b.at[j, 1], j, 5)
        a = term_a[j, x].astype(F32) + rs_a[j, 0].astype(F32) + rs_a[j, 1].astype(F32)
        b = term_b[j, x].astype(F32) + rs_b[j, 0].astype(F32) + rs_b[j, 1].astype(F32)
        ret_a[NZ // CH * j : NZ // CH * (j + 1)] = a.astype(BF16).reshape(NZ // CH, NG * CAP, H)
        total_b.append(b.astype(BF16))
    total_b = jnp.concatenate(total_b, axis=0)

    exchange(2, z_peers, z, ret_a, hop_a, z_s, z_r)
    ret_b[...] = dot(to_gz[...], total_b).astype(BF16).reshape(NG, NZ * CAP, H)
    exchange(2, g_peers, g, ret_b, hop_b, g_s, g_r)
    hop_a[z] = ret_a[z]
    hop_b[g] = ret_b[g]
    all_arrived(2, z_peers, ret_a, hop_a, z_s, z_r)
    mid_a[...] = dot(to_gz[...], hop_a[...].reshape(ROWS, H)).astype(BF16).reshape(NG, NZ * CAP, H)
    exchange(3, g_peers, g, mid_a, back_a, g_s, g_r)
    all_arrived(2, g_peers, ret_b, hop_b, g_s, g_r)
    mid_b[...] = dot(to_zg[...], hop_b[...].reshape(ROWS, H)).astype(BF16).reshape(NZ, NG * CAP, H)
    exchange(3, z_peers, z, mid_b, back_b, z_s, z_r)
    back_a[g] = mid_a[g]
    back_b[z] = mid_b[z]
    all_arrived(3, g_peers, mid_a, back_a, g_s, g_r)
    all_arrived(3, z_peers, mid_b, back_b, z_s, z_r)
    for half, comb, back in ((0, comb_a, back_a), (1, comb_b, back_b)):
        rows = back[...].reshape(ROWS, H)
        moe = dot(comb[:, 0:ROWS], rows) + dot(comb[:, ROWS:], rows)
        at = slice(H * half, H * half + H)
        mixed_out[:, at] = (resid[:, at].astype(F32) + moe).astype(BF16)

    for copy in sends:
        copy.wait_send()


def body(
    tokens,
    conv_state,
    lru_state,
    mix_gain,
    ffn_gain,
    w_branch,
    w_gate,
    conv_taps,
    w_recur,
    w_inject,
    lru_lambda,
    w_out,
    expert_gate,
    expert_up,
    expert_down,
    route_ids,
    route_weight,
):
    conv_state = jnp.transpose(conv_state, (1, 0, 2))
    route_ids = jnp.transpose(route_ids)
    route_weight = jnp.transpose(route_weight)
    lru_lambda = lru_lambda.reshape(1, H)
    mix_gain = mix_gain.reshape(1, D)
    ffn_gain = ffn_gain.reshape(1, D)
    operands = (
        tokens,
        conv_state,
        lru_state,
        mix_gain,
        ffn_gain,
        w_branch,
        w_gate,
        conv_taps,
        w_recur,
        w_inject,
        lru_lambda,
        w_out,
        expert_gate,
        expert_up,
        expert_down,
        route_ids,
        route_weight,
    )

    def vm(*shape, dtype=BF16):
        return pltpu.VMEM(shape, dtype)

    landing = [vm(NX, S, F)]
    landing += [pltpu.VMEM(a.shape, a.dtype) for a in operands[1:]]
    by_g = (NG, NZ * CAP, H)
    by_z = (NZ, NG * CAP, H)
    scratch = landing + [
        vm(H, 2 * H),
        vm(ROWS, S),
        vm(ROWS, S),
        vm(S, 2 * ROWS),
        vm(S, 2 * ROWS),
        vm(ROWS, ROWS),
        vm(ROWS, ROWS),
        vm(NX, S, F),
        vm(NX, S, F),
        vm(*by_g),
        vm(*by_z),
        vm(*by_g),
        vm(*by_z),
        vm(*by_z),
        vm(*by_g),
        vm(NX, *by_z),
        vm(NX, *by_g),
        vm(ROWS, D),
        vm(CH, NX, CR, H),
        vm(CH, NX, CR, H),
        vm(CH, CR, H),
        vm(CH, CR, H),
        vm(CH, CR, H),
        vm(CH, CR, H),
        vm(CH, 2, CR, H),
        vm(CH, 2, CR, H),
        vm(*by_z),
        vm(*by_g),
        vm(*by_z),
        vm(*by_g),
        vm(*by_g),
        vm(*by_z),
        vm(*by_g),
        vm(*by_z),
    ]
    dma = pltpu.SemaphoreType.DMA
    scratch += [
        dma((17,)),
        dma((NX,)),
        dma((NX,)),
        dma((NX,)),
        dma((NX,)),
        dma((4, NG)),
        dma((4, NG)),
        dma((4, NZ)),
        dma((4, NZ)),
        dma((3, NZ)),
        dma((NX, NZ)),
        dma((3, NZ)),
        dma((NX, NZ)),
        dma((CH, 6)),
        dma((CH, 6)),
    ]
    return pl.pallas_call(
        kernel,
        out_shape=(
            jax.ShapeDtypeStruct((S, F), BF16),
            jax.ShapeDtypeStruct((S, H), F32),
        ),
        in_specs=[pl.BlockSpec(memory_space=pltpu.HBM)] * len(operands),
        out_specs=(
            pl.BlockSpec(memory_space=pltpu.VMEM),
            pl.BlockSpec(memory_space=pltpu.VMEM),
        ),
        scratch_shapes=scratch,
        compiler_params=pltpu.CompilerParams(
            collective_id=0, has_side_effects=True, vmem_limit_bytes=67043328
        ),
        name="layer",
    )(*operands)


def solution(mesh):
    placed = (
        P("ep", "tp"),
        P("ep", None, "tp"),
        P("ep", "tp"),
        P(),
        P(),
        P(None, "tp"),
        P(None, "tp"),
        P(None, "tp"),
        P("tp", None, None),
        P("tp", None, None),
        P("tp"),
        P("tp", None),
        P("ep", None, "tp"),
        P("ep", None, "tp"),
        P("ep", "tp", None),
        P("ep", None),
        P("ep", None),
    )
    return jax.shard_map(
        body, mesh=mesh, in_specs=placed, out_specs=(P("ep", "tp"), P("ep", "tp")), check_vma=False
    )
```

```python
import functools

import jax
import jax.numpy as jnp
from jax import lax
from jax.experimental import pallas as pl
from jax.experimental.pallas import tpu as pltpu
from jax.sharding import PartitionSpec as P

EPS = 1e-06
LRU_SCALE = 8.0
MESH = pl.DeviceIdType.MESH
F32 = jnp.float32
BF16 = jnp.bfloat16

NX = 4
NZ = 8
NG = 16
S = 64
CAP = 2
F = 256
H = 128
ROWS = NZ * NG * CAP
D = NX * F
HALF = ROWS // 2
EARLY = 5

RING8 = (4, 3, 5, 2, 6, 1, 7)
STEPS = (0, 1, 7, 2, 6, 3, 5, 4)


def remote(src, dst, send, recv, dev):
    return pltpu.make_async_remote_copy(
        src_ref=src, dst_ref=dst, send_sem=send, recv_sem=recv, device_id=dev, device_id_type=MESH
    )


def iota(shape, dim):
    return lax.broadcasted_iota(jnp.int32, shape, dim)


def dot(a, b):
    return jnp.dot(a, b, preferred_element_type=F32)


def swap_matrix(outer, inner):
    row = iota((ROWS, ROWS), 0)
    col = iota((ROWS, ROWS), 1)
    slot = lax.rem(row, CAP)
    mid = lax.rem(lax.div(row, CAP), inner)
    top = lax.div(row, CAP * inner)
    source = mid * (outer * CAP) + top * CAP + slot
    return jnp.where(col == source, 1.0, 0.0).astype(BF16)


def rank(offset):
    back = 2 * (8 - offset)
    return jnp.where(offset == 0, 0, jnp.where(offset <= 4, 2 * offset - 1, back))


def place_b(i, z, y):
    j = lax.div(i, NG * CAP)
    offset = jnp.where(lax.rem(j, 2) == 1, lax.div(j + 1, 2), 8 - lax.div(j, 2))
    at_z = lax.rem(z + offset, NZ)
    at_g = lax.rem(lax.div(i, CAP), NG)
    step = rank(lax.rem(lax.div(at_g, 2) + 8 - y, 8))
    return (step * 2 + lax.rem(at_g, 2)) * (NZ * CAP) + at_z * CAP + lax.rem(i, CAP)


def kernel(
    tokens,
    conv_state,
    lru_state,
    mix_gain,
    ffn_gain,
    w_branch,
    w_gate,
    conv_taps,
    w_recur,
    w_inject,
    lru_lambda,
    w_out,
    expert_gate,
    expert_up,
    expert_down,
    ids,
    weights,
    mixed_out,
    state_out,
    xg,
    conv_v,
    lru_v,
    mixg_v,
    ffng_v,
    wb_v,
    wg_v,
    taps_v,
    wr_v,
    wi_v,
    lam_v,
    wo_v,
    eg_v,
    eu_v,
    ed_v,
    ids_v,
    rw_v,
    bd,
    pick_a,
    pick_b,
    comb_a,
    comb_b,
    to_zg,
    to_gz,
    to_a,
    to_b,
    part,
    mr,
    send_a,
    send_b,
    got_a,
    got_b,
    fwd_a,
    fwd_b,
    all_a,
    all_b,
    gains,
    acc_g,
    acc_u,
    term_a,
    term_b,
    rel_a,
    rel_b,
    sum_a,
    sum_b,
    rs_a,
    rs_b,
    ret_a,
    ret_b,
    hop_a,
    hop_b,
    mid_a,
    mid_b,
    back_a,
    back_b,
    in_sem,
    x_sem,
    g_s,
    g_r,
    z_s,
    z_r,
    ax_s,
    bx_s,
    ax_step,
    bx_step,
    x_r,
    rs_s,
    rs_r,
):
    x = lax.axis_index("tp")
    e = lax.axis_index("ep")
    z = lax.div(e, NG)
    g = lax.rem(e, NG)
    y = lax.div(g, 2)
    c = lax.rem(g, 2)

    x_dev = [(e, lax.rem(x + d, NX)) for d in range(NX)]
    x_idx = [lax.rem(x + d, NX) for d in range(NX)]
    z_peers = []
    for dz in RING8:
        i = lax.rem(z + dz, NZ)
        z_peers.append((i, (i * NG + g, x)))
    g_peers = []
    for dy in RING8 + (0,):
        for dc in (0, 1):
            if dy or dc:
                i = lax.rem(y + dy, 8) * 2 + lax.rem(c + dc, 2)
                g_peers.append((i, (z * NG + i, x)))

    z_ring, g_ring = [], []
    for dy in STEPS[::-1]:
        place = STEPS.index(-dy % 8)
        if dy:
            i = lax.rem(z + dy, NZ)
            z_ring.append((place, i, (i * NG + g, x)))
        for dc in (1, 0):
            if dy or dc:
                i = lax.rem(y + dy, 8) * 2 + lax.rem(c + dc, 2)
                g_ring.append((place, i, (z * NG + i, x)))

    barrier = pltpu.get_barrier_semaphore()
    for _, dev in z_peers + g_peers:
        pl.semaphore_signal(barrier, inc=1, device_id=dev, device_id_type=MESH)
    for dev in x_dev[1:]:
        pl.semaphore_signal(barrier, inc=1, device_id=dev, device_id_type=MESH)

    loads = {}
    pairs = (
        ("tok", tokens, xg.at[x]),
        ("ids", ids, ids_v),
        ("rw", weights, rw_v),
        ("mixg", mix_gain, mixg_v),
        ("conv", conv_state, conv_v),
        ("taps", conv_taps, taps_v),
        ("wb", w_branch, wb_v),
        ("wg", w_gate, wg_v),
        ("wr", w_recur, wr_v),
        ("wi", w_inject, wi_v),
        ("lam", lru_lambda, lam_v),
        ("lru", lru_state, lru_v),
        ("wo", w_out, wo_v),
        ("ffng", ffn_gain, ffng_v),
        ("eg", expert_gate, eg_v),
        ("eu", expert_up, eu_v),
        ("ed", expert_down, ed_v),
    )
    for i, (name, src, dst) in enumerate(pairs):
        loads[name] = pltpu.make_async_copy(src, dst, in_sem.at[i])
        loads[name].start()

    loads["tok"].wait()
    pl.semaphore_wait(barrier, len(z_peers) + len(g_peers) + NX - 1)

    near = x_dev[1]

    def got(dst, sem):
        remote(dst, dst, sem, sem, near).wait_recv()

    def sent(src, sem):
        remote(src, src, sem, sem, near).wait_send()

    for d in (2, 1, 3):
        remote(xg.at[x], xg.at[x], x_sem.at[0], x_sem.at[1], x_dev[d]).start()

    loads["ids"].wait()
    loads["rw"].wait()
    for pick, comb, outer, inner in ((pick_a, comb_a, NG, NZ), (pick_b, comb_b, NZ, NG)):
        row = iota((ROWS, S), 0)
        slot = lax.rem(row, CAP).astype(F32)
        first = lax.rem(lax.div(row, CAP), inner)
        second = lax.div(row, CAP * inner)
        expert = first * NG + second if outer == NG else second * NG + first
        hit0 = jnp.where(ids_v[0:1, :] == expert, 1.0, 0.0)
        hit1 = jnp.where(ids_v[1:2, :] == expert, 1.0, 0.0)
        hit = hit0 + hit1
        earlier = jnp.where(iota((S, S), 0) < iota((S, S), 1), 1.0, 0.0).astype(BF16)
        before = dot(hit.astype(BF16), earlier)
        chosen = jnp.where(before == slot, hit, 0.0)
        pick[...] = chosen.astype(BF16)
        weight = jnp.where(before == slot, hit0 * rw_v[0:1, :] + hit1 * rw_v[1:2, :], 0.0)
        weight = jnp.transpose(weight)
        high = weight.astype(BF16)
        comb[:, 0:ROWS] = high
        comb[:, ROWS:] = (weight - high.astype(F32)).astype(BF16)
    to_zg[...] = swap_matrix(NZ, NG)
    to_gz[...] = swap_matrix(NG, NZ)
    row, col = iota((ROWS, ROWS), 0), iota((ROWS, ROWS), 1)
    to_a[...] = jnp.where(place_b(row, z, y) == col, 1.0, 0.0).astype(BF16)
    to_b[...] = jnp.where(place_b(col, z, y) == row, 1.0, 0.0).astype(BF16)

    loads["wr"].wait()
    loads["wi"].wait()
    bd[...] = jnp.zeros_like(bd)
    for h in range(2):
        lo, hi = 64 * h, 64 * h + 64
        for k, w in enumerate((wr_v, wi_v)):
            bd[lo:hi, H * k + lo : H * k + hi] = w[h]
    loads["conv"].wait()
    loads["taps"].wait()
    taps = taps_v[...].astype(F32)
    old = (
        conv_v[0].astype(F32) * taps[0:1]
        + conv_v[1].astype(F32) * taps[1:2]
        + conv_v[2].astype(F32) * taps[2:3]
    )
    loads["lam"].wait()
    decay = -LRU_SCALE * jax.nn.softplus(-lam_v[...])
    loads["lru"].wait()
    loads["mixg"].wait()
    gain = mixg_v[...].reshape(1, D).astype(F32)
    for name in ("wb", "wg", "wo"):
        loads[name].wait()

    got(xg.at[pl.ds(0, NX - 1)], x_sem.at[1])
    whole = jnp.concatenate([xg[k].astype(F32) for k in range(NX)], axis=1)
    scale = lax.rsqrt(jnp.sum(whole * whole, axis=1, keepdims=True) * (1.0 / D) + EPS)
    normed = (whole * scale * gain).astype(BF16)
    branch = dot(normed, wb_v[...]).astype(BF16)
    gate_in = dot(normed, wg_v[...]).astype(BF16).astype(F32)
    conv_out = old + branch.astype(F32) * taps[3:4]
    gates = jax.nn.sigmoid(dot(conv_out.astype(BF16), bd[...]))
    recur, inject = gates[:, :H], gates[:, H:]
    log_decay = recur * decay
    state = (
        jnp.exp(log_decay) * lru_v[...]
        + jnp.sqrt(1.0 - jnp.exp(2.0 * log_decay)) * inject * conv_out
    )
    state_out[...] = state
    lru_out = (state * jax.nn.gelu(gate_in)).astype(BF16)
    partial = dot(lru_out, wo_v[...]).astype(BF16)
    for k in range(NX):
        part[k] = partial[:, F * k : F * k + F]
    for d in (2, 1, 3):
        remote(part.at[x_idx[d]], mr.at[x], x_sem.at[2], x_sem.at[3], x_dev[d]).start()
    mix = part[x].astype(F32)
    got(mr.at[pl.ds(0, NX - 1)], x_sem.at[3])
    for d in (1, 3, 2):
        mix = mix + mr[x_idx[d]].astype(F32)
    resid = (xg[x].astype(F32) + mix.astype(BF16).astype(F32)).astype(BF16)

    def exchange(way, peers, own, src, dst, s, r):
        for p, dev in peers:
            remote(src.at[p], dst.at[own], s.at[way], r.at[way], dev).start()

    def all_arrived(way, peers, dst, r):
        got(dst.at[pl.ds(0, len(peers))], r.at[way])

    send_a[...] = dot(pick_a[...], resid[:, :H]).astype(BF16).reshape(NG, NZ * CAP, H)
    exchange(0, g_peers, g, send_a, got_a, g_s, g_r)
    send_b[...] = dot(pick_b[...], resid[:, H:]).astype(BF16).reshape(NZ, NG * CAP, H)
    exchange(0, z_peers, z, send_b, got_b, z_s, z_r)
    got_a[g] = send_a[g]
    got_b[z] = send_b[z]
    all_arrived(0, z_peers, got_b, z_r)
    fwd_b[...] = dot(to_gz[...], got_b[...].reshape(ROWS, H)).astype(BF16).reshape(NG, NZ * CAP, H)
    for j, p, dev in g_ring[::-1]:
        remote(fwd_b.at[p], all_b.at[x, 2 * j + c], g_s.at[3], g_r.at[3 + j], dev).start()
    all_arrived(0, g_peers, got_a, g_r)
    fwd_a[...] = dot(to_zg[...], got_a[...].reshape(ROWS, H)).astype(BF16).reshape(NZ, NG * CAP, H)
    for j, p, dev in z_ring[::-1]:
        remote(fwd_a.at[p], all_a.at[x, j], z_s.at[3], z_r.at[3 + j], dev).start()
    all_a[x, 0] = fwd_a[z]
    all_b[x, c] = fwd_b[g]

    left, half_way, right = x_idx[3], x_idx[2], x_idx[1]

    def pass_on(j):
        a, b = all_a.at[x, j], all_b.at[x, pl.ds(2 * j, 2)]
        if j >= EARLY:
            remote(a, a, ax_s.at[3], x_r.at[4], x_dev[2]).start()
            remote(b, b, bx_s.at[3], x_r.at[5], x_dev[2]).start()
        remote(a, a, ax_s.at[0], ax_step.at[j], x_dev[1]).start()
        remote(b, b, bx_s.at[0], bx_step.at[j], x_dev[3]).start()
        if j < 3:
            remote(a, a, ax_s.at[1], x_r.at[0], x_dev[3]).start()
            remote(b, b, bx_s.at[1], x_r.at[1], x_dev[1]).start()

    for j in range(NZ):
        if j:
            got(all_a.at[x, j], z_r.at[3 + j])
            got(all_b.at[x, pl.ds(2 * j, 2)], g_r.at[3 + j])
        else:
            got(all_b.at[x, 0], g_r.at[3])
        pass_on(j)
    a, b = all_a.at[x, pl.ds(3, NZ - 3)], all_b.at[x, pl.ds(6, 2 * NZ - 6)]
    remote(a, a, ax_s.at[1], x_r.at[0], x_dev[3]).start()
    remote(b, b, bx_s.at[1], x_r.at[1], x_dev[1]).start()
    for j in range(EARLY):
        a, b = all_a.at[left, j], all_b.at[right, pl.ds(2 * j, 2)]
        got(a, ax_step.at[j])
        remote(a, a, ax_s.at[2], x_r.at[2], x_dev[1]).start()
        got(b, bx_step.at[j])
        remote(b, b, bx_s.at[2], x_r.at[3], x_dev[3]).start()

    loads["ffng"].wait()
    gain = ffng_v[...].reshape(1, D).astype(F32)
    for k in range(NX):
        gains[k] = gain[:, F * k : F * k + F]
    for name in ("eg", "eu", "ed"):
        loads[name].wait()
    squares = jnp.zeros((ROWS, H), F32)
    for n, k in enumerate((x, left, right, half_way)):
        if n == 1:
            for j in range(EARLY, NZ):
                got(all_a.at[left, j], ax_step.at[j])
            got(all_b.at[left], x_r.at[1])
        if n == 2:
            for j in range(EARLY, NZ):
                got(all_b.at[right, pl.ds(2 * j, 2)], bx_step.at[j])
            got(all_a.at[right], x_r.at[0])
        if n == 3:
            got(all_a.at[k, pl.ds(0, EARLY)], x_r.at[2])
            got(all_b.at[k, pl.ds(0, 2 * EARLY)], x_r.at[3])
            got(all_a.at[k, pl.ds(EARLY, NZ - EARLY)], x_r.at[4])
            got(all_b.at[k, pl.ds(2 * EARLY, 2 * (NZ - EARLY))], x_r.at[5])
        a = all_a[k].reshape(ROWS, H).astype(F32)
        b = dot(to_a[...], all_b[k].reshape(ROWS, H))
        squares = squares + a * a + b * b
        rows = (jnp.concatenate([a, b], axis=1) * gains[k]).astype(BF16)
        at = pl.ds(pl.multiple_of(k * F, F), F)
        first = dot(rows, eg_v[0, at, :])
        second = dot(rows, eu_v[0, at, :])
        if n == 0:
            acc_g[...] = first
            acc_u[...] = second
        elif n < 3:
            acc_g[...] += first
            acc_u[...] += second
    scale = lax.rsqrt(jnp.sum(squares, axis=1, keepdims=True) * (1.0 / D) + EPS)
    first = (acc_g[...] + first) * scale
    second = (acc_u[...] + second) * scale
    hidden = (first * jax.nn.sigmoid(first) * second).astype(BF16)

    def down(k):
        at = pl.ds(pl.multiple_of(k * F, F), F)
        term = dot(hidden, ed_v[0, :, at]).astype(BF16)
        b = dot(to_b[...], term[:, H:]).astype(BF16)
        for j, rows in enumerate((slice(HALF, ROWS), slice(0, HALF))):
            term_a[j, k] = term[rows, :H]
            term_b[j, k] = b[rows]

    def send_term(j, src, dst, lane, dev):
        remote(src, dst, rs_s.at[j, 0], rs_r.at[j, lane], dev).start()

    down(half_way)
    for j in range(2):
        send_term(j, term_a.at[j, half_way], rel_a.at[j], 0, x_dev[1])
        send_term(j, term_b.at[j, half_way], rel_b.at[j], 1, x_dev[3])
    down(right)
    down(left)
    for j in range(2):
        send_term(j, term_b.at[j, right], rs_b.at[j, 0], 2, x_dev[1])
        send_term(j, term_a.at[j, left], rs_a.at[j, 0], 3, x_dev[3])
    down(x)

    def landed(dst, j, lane):
        got(dst, rs_r.at[j, lane])

    def halfway(j):
        landed(rel_a.at[j], j, 0)
        sum_a[j] = (term_a[j, right].astype(F32) + rel_a[j].astype(F32)).astype(BF16)
        remote(sum_a.at[j], rs_a.at[j, 1], rs_s.at[j, 1], rs_r.at[j, 4], x_dev[1]).start()
        landed(rel_b.at[j], j, 1)
        sum_b[j] = (term_b[j, left].astype(F32) + rel_b[j].astype(F32)).astype(BF16)
        remote(sum_b.at[j], rs_b.at[j, 1], rs_s.at[j, 1], rs_r.at[j, 5], x_dev[3]).start()

    halfway(0)
    halfway(1)
    for j, lo in ((0, NZ // 2), (1, 0)):
        landed(rs_a.at[j, 0], j, 3)
        landed(rs_b.at[j, 0], j, 2)
        landed(rs_a.at[j, 1], j, 4)
        landed(rs_b.at[j, 1], j, 5)
        a = term_a[j, x].astype(F32) + rs_a[j, 0].astype(F32) + rs_a[j, 1].astype(F32)
        b = term_b[j, x].astype(F32) + rs_b[j, 0].astype(F32) + rs_b[j, 1].astype(F32)
        ret_a[lo : lo + NZ // 2] = a.astype(BF16).reshape(NZ // 2, NG * CAP, H)
        ret_b[2 * lo : 2 * lo + NZ] = b.astype(BF16).reshape(NZ, NZ * CAP, H)
        for place in range(lo + NZ // 2 - 1, lo - 1, -1):
            i = lax.rem(z + STEPS[place], NZ)
            if place:
                remote(ret_a.at[place], hop_a.at[z], z_s.at[1], z_r.at[1], (i * NG + g, x)).start()
            for dc in (1, 0):
                if place or dc:
                    core = lax.rem(c + dc, 2)
                    i = lax.rem(y + STEPS[place], 8) * 2 + core
                    src = ret_b.at[2 * place + core]
                    remote(src, hop_b.at[g], g_s.at[1], g_r.at[1], (z * NG + i, x)).start()
    hop_a[z] = ret_a[0]
    hop_b[g] = ret_b[c]
    all_arrived(1, z_peers, hop_a, z_r)
    mid_a[...] = dot(to_gz[...], hop_a[...].reshape(ROWS, H)).astype(BF16).reshape(NG, NZ * CAP, H)
    exchange(2, g_peers, g, mid_a, back_a, g_s, g_r)
    all_arrived(1, g_peers, hop_b, g_r)
    mid_b[...] = dot(to_zg[...], hop_b[...].reshape(ROWS, H)).astype(BF16).reshape(NZ, NG * CAP, H)
    exchange(2, z_peers, z, mid_b, back_b, z_s, z_r)
    back_a[g] = mid_a[g]
    back_b[z] = mid_b[z]
    all_arrived(2, g_peers, back_a, g_r)
    all_arrived(2, z_peers, back_b, z_r)
    for half, comb, back in ((0, comb_a, back_a), (1, comb_b, back_b)):
        rows = back[...].reshape(ROWS, H)
        moe = dot(comb[:, 0:ROWS], rows) + dot(comb[:, ROWS:], rows)
        at = slice(H * half, H * half + H)
        mixed_out[:, at] = (resid[:, at].astype(F32) + moe).astype(BF16)

    sent(xg.at[pl.ds(0, NX - 1)], x_sem.at[0])
    sent(part.at[pl.ds(0, NX - 1)], x_sem.at[2])
    for way in range(4):
        sent(send_a.at[pl.ds(0, NG - 1)], g_s.at[way])
        sent(send_b.at[pl.ds(0, NZ - 1)], z_s.at[way])
    for lane in range(2):
        sent(all_a.at[0], ax_s.at[lane])
        sent(all_b.at[0], bx_s.at[lane])
    sent(all_a.at[0, pl.ds(0, EARLY)], ax_s.at[2])
    sent(all_b.at[0, pl.ds(0, 2 * EARLY)], bx_s.at[2])
    sent(all_a.at[0, pl.ds(EARLY, NZ - EARLY)], ax_s.at[3])
    sent(all_b.at[0, pl.ds(2 * EARLY, 2 * (NZ - EARLY))], bx_s.at[3])
    for j in range(2):
        sent(term_a.at[0], rs_s.at[j, 0])
        sent(rs_a.at[0], rs_s.at[j, 1])


def body(
    tokens,
    conv_state,
    lru_state,
    mix_gain,
    ffn_gain,
    w_branch,
    w_gate,
    conv_taps,
    w_recur,
    w_inject,
    lru_lambda,
    w_out,
    expert_gate,
    expert_up,
    expert_down,
    route_ids,
    route_weight,
):
    conv_state = jnp.transpose(conv_state, (1, 0, 2))
    route_ids = jnp.transpose(route_ids)
    route_weight = jnp.transpose(route_weight)
    lru_lambda = lru_lambda.reshape(1, H)
    operands = (
        tokens,
        conv_state,
        lru_state,
        mix_gain,
        ffn_gain,
        w_branch,
        w_gate,
        conv_taps,
        w_recur,
        w_inject,
        lru_lambda,
        w_out,
        expert_gate,
        expert_up,
        expert_down,
        route_ids,
        route_weight,
    )

    operands = tuple(pltpu.with_memory_space_constraint(a, pltpu.HBM) for a in operands)

    def vm(*shape, dtype=BF16):
        return pltpu.VMEM(shape, dtype)

    landing = [vm(NX, S, F)]
    landing += [pltpu.VMEM(a.shape, a.dtype) for a in operands[1:]]
    by_g = (NG, NZ * CAP, H)
    by_z = (NZ, NG * CAP, H)
    scratch = landing + [
        vm(H, 2 * H),
        vm(ROWS, S),
        vm(ROWS, S),
        vm(S, 2 * ROWS),
        vm(S, 2 * ROWS),
        vm(ROWS, ROWS),
        vm(ROWS, ROWS),
        vm(ROWS, ROWS),
        vm(ROWS, ROWS),
        vm(NX, S, F),
        vm(NX, S, F),
        vm(*by_g),
        vm(*by_z),
        vm(*by_g),
        vm(*by_z),
        vm(*by_z),
        vm(*by_g),
        vm(NX, *by_z),
        vm(NX, *by_g),
        vm(NX, 1, F, dtype=F32),
        vm(ROWS, expert_gate.shape[2], dtype=F32),
        vm(ROWS, expert_gate.shape[2], dtype=F32),
        vm(2, NX, HALF, H),
        vm(2, NX, HALF, H),
        vm(2, HALF, H),
        vm(2, HALF, H),
        vm(2, HALF, H),
        vm(2, HALF, H),
        vm(2, 2, HALF, H),
        vm(2, 2, HALF, H),
        vm(*by_z),
        vm(*by_g),
        vm(*by_z),
        vm(*by_g),
        vm(*by_g),
        vm(*by_z),
        vm(*by_g),
        vm(*by_z),
    ]
    dma = pltpu.SemaphoreType.DMA
    scratch += [
        dma((17,)),
        dma((4,)),
        dma((4,)),
        dma((3 + NZ,)),
        dma((4,)),
        dma((3 + NZ,)),
        dma((4,)),
        dma((4,)),
        dma((NZ,)),
        dma((NZ,)),
        dma((6,)),
        dma((2, 2)),
        dma((2, 6)),
    ]
    return pl.pallas_call(
        kernel,
        out_shape=(
            jax.ShapeDtypeStruct((S, F), BF16),
            jax.ShapeDtypeStruct((S, H), F32),
        ),
        in_specs=[pl.BlockSpec(memory_space=pltpu.HBM)] * len(operands),
        out_specs=(
            pl.BlockSpec(memory_space=pltpu.VMEM),
            pl.BlockSpec(memory_space=pltpu.VMEM),
        ),
        scratch_shapes=scratch,
        compiler_params=pltpu.CompilerParams(
            collective_id=0, has_side_effects=True, vmem_limit_bytes=33554432
        ),
        name="layer",
    )(*operands)


def solution(mesh):
    placed = (
        P("ep", "tp"),
        P("ep", None, "tp"),
        P("ep", "tp"),
        P(),
        P(),
        P(None, "tp"),
        P(None, "tp"),
        P(None, "tp"),
        P("tp", None, None),
        P("tp", None, None),
        P("tp"),
        P("tp", None),
        P("ep", None, "tp"),
        P("ep", None, "tp"),
        P("ep", "tp", None),
        P("ep", None),
        P("ep", None),
    )
    return jax.shard_map(
        body, mesh=mesh, in_specs=placed, out_specs=(P("ep", "tp"), P("ep", "tp")), check_vma=False
    )
```

```python
import functools

import jax
import jax.numpy as jnp
from jax import lax
from jax.experimental import pallas as pl
from jax.experimental.pallas import tpu as pltpu
from jax.sharding import PartitionSpec as P

EPS = 1e-06
LRU_SCALE = 8.0
MESH = pl.DeviceIdType.MESH
F32 = jnp.float32
BF16 = jnp.bfloat16

NX = 4
NZ = 8
NG = 16
S = 64
CAP = 2
F = 256
H = 128
ROWS = NZ * NG * CAP
D = NX * F

RING8 = (4, 3, 5, 2, 6, 1, 7)


def remote(src, dst, send, recv, dev):
    return pltpu.make_async_remote_copy(
        src_ref=src, dst_ref=dst, send_sem=send, recv_sem=recv, device_id=dev, device_id_type=MESH
    )


def iota(shape, dim):
    return lax.broadcasted_iota(jnp.int32, shape, dim)


def dot(a, b):
    return jnp.dot(a, b, preferred_element_type=F32)


def swap_matrix(outer, inner):
    row = iota((ROWS, ROWS), 0)
    col = iota((ROWS, ROWS), 1)
    slot = lax.rem(row, CAP)
    mid = lax.rem(lax.div(row, CAP), inner)
    top = lax.div(row, CAP * inner)
    source = mid * (outer * CAP) + top * CAP + slot
    return jnp.where(col == source, 1.0, 0.0).astype(BF16)


def kernel(
    tokens,
    conv_state,
    lru_state,
    mix_gain,
    ffn_gain,
    w_branch,
    w_gate,
    conv_taps,
    w_recur,
    w_inject,
    lru_lambda,
    w_out,
    expert_gate,
    expert_up,
    expert_down,
    ids,
    weights,
    mixed_out,
    state_out,
    xg,
    conv_v,
    lru_v,
    mixg_v,
    ffng_v,
    wb_v,
    wg_v,
    taps_v,
    wr_v,
    wi_v,
    lam_v,
    wo_v,
    eg_v,
    eu_v,
    ed_v,
    ids_v,
    rw_v,
    bd,
    pick_a,
    pick_b,
    comb_a,
    comb_b,
    to_zg,
    to_gz,
    part,
    mr,
    send_a,
    send_b,
    got_a,
    got_b,
    fwd_a,
    fwd_b,
    all_a,
    all_b,
    gains,
    acc_g,
    acc_u,
    term_a,
    term_b,
    hop_a,
    hop_b,
    mid_a,
    mid_b,
    back_a,
    back_b,
    in_sem,
    x_sem,
    g_s,
    g_r,
    z_s,
    z_r,
    shard_a,
    shard_b,
):
    x = lax.axis_index("tp")
    e = lax.axis_index("ep")
    z = lax.div(e, NG)
    g = lax.rem(e, NG)
    y = lax.div(g, 2)
    c = lax.rem(g, 2)

    x_dev = [(e, lax.rem(x + d, NX)) for d in range(NX)]
    x_idx = [lax.rem(x + d, NX) for d in range(NX)]
    z_peers = []
    for dz in RING8:
        i = lax.rem(z + dz, NZ)
        z_peers.append((i, (i * NG + g, x)))
    g_peers = []
    for dy in RING8 + (0,):
        for dc in (0, 1):
            if dy or dc:
                i = lax.rem(y + dy, 8) * 2 + lax.rem(c + dc, 2)
                g_peers.append((i, (z * NG + i, x)))

    barrier = pltpu.get_barrier_semaphore()
    for _, dev in z_peers + g_peers:
        pl.semaphore_signal(barrier, inc=1, device_id=dev, device_id_type=MESH)
    for dev in x_dev[1:]:
        pl.semaphore_signal(barrier, inc=1, device_id=dev, device_id_type=MESH)

    loads = {}
    pairs = (
        ("tok", tokens, xg.at[x]),
        ("ids", ids, ids_v),
        ("rw", weights, rw_v),
        ("mixg", mix_gain, mixg_v),
        ("conv", conv_state, conv_v),
        ("taps", conv_taps, taps_v),
        ("wb", w_branch, wb_v),
        ("wg", w_gate, wg_v),
        ("wr", w_recur, wr_v),
        ("wi", w_inject, wi_v),
        ("lam", lru_lambda, lam_v),
        ("lru", lru_state, lru_v),
        ("wo", w_out, wo_v),
        ("ffng", ffn_gain, ffng_v),
        ("eg", expert_gate, eg_v),
        ("eu", expert_up, eu_v),
        ("ed", expert_down, ed_v),
    )
    for i, (name, src, dst) in enumerate(pairs):
        loads[name] = pltpu.make_async_copy(src, dst, in_sem.at[i])
        loads[name].start()

    loads["tok"].wait()
    pl.semaphore_wait(barrier, len(z_peers) + len(g_peers) + NX - 1)

    near = x_dev[1]

    def got(dst, sem):
        remote(dst, dst, sem, sem, near).wait_recv()

    def sent(src, sem):
        remote(src, src, sem, sem, near).wait_send()

    for d in (2, 1, 3):
        remote(xg.at[x], xg.at[x], x_sem.at[0], x_sem.at[1], x_dev[d]).start()

    loads["ids"].wait()
    loads["rw"].wait()
    for pick, comb, outer, inner in ((pick_a, comb_a, NG, NZ), (pick_b, comb_b, NZ, NG)):
        row = iota((ROWS, S), 0)
        slot = lax.rem(row, CAP).astype(F32)
        first = lax.rem(lax.div(row, CAP), inner)
        second = lax.div(row, CAP * inner)
        expert = first * NG + second if outer == NG else second * NG + first
        hit0 = jnp.where(ids_v[0:1, :] == expert, 1.0, 0.0)
        hit1 = jnp.where(ids_v[1:2, :] == expert, 1.0, 0.0)
        hit = hit0 + hit1
        earlier = jnp.where(iota((S, S), 0) < iota((S, S), 1), 1.0, 0.0).astype(BF16)
        before = dot(hit.astype(BF16), earlier)
        chosen = jnp.where(before == slot, hit, 0.0)
        pick[...] = chosen.astype(BF16)
        weight = jnp.where(before == slot, hit0 * rw_v[0:1, :] + hit1 * rw_v[1:2, :], 0.0)
        weight = jnp.transpose(weight)
        high = weight.astype(BF16)
        comb[:, 0:ROWS] = high
        comb[:, ROWS:] = (weight - high.astype(F32)).astype(BF16)
    to_zg[...] = swap_matrix(NZ, NG)
    to_gz[...] = swap_matrix(NG, NZ)

    loads["wr"].wait()
    loads["wi"].wait()
    bd[...] = jnp.zeros_like(bd)
    for h in range(2):
        lo, hi = 64 * h, 64 * h + 64
        for k, w in enumerate((wr_v, wi_v)):
            bd[lo:hi, H * k + lo : H * k + hi] = w[h]
    loads["conv"].wait()
    loads["taps"].wait()
    taps = taps_v[...].astype(F32)
    old = (
        conv_v[0].astype(F32) * taps[0:1]
        + conv_v[1].astype(F32) * taps[1:2]
        + conv_v[2].astype(F32) * taps[2:3]
    )
    loads["lam"].wait()
    decay = -LRU_SCALE * jax.nn.softplus(-lam_v[...])
    loads["lru"].wait()
    loads["mixg"].wait()
    gain = mixg_v[...].reshape(1, D).astype(F32)
    for name in ("wb", "wg", "wo"):
        loads[name].wait()

    got(xg.at[pl.ds(0, NX - 1)], x_sem.at[1])
    whole = jnp.concatenate([xg[k].astype(F32) for k in range(NX)], axis=1)
    scale = lax.rsqrt(jnp.sum(whole * whole, axis=1, keepdims=True) * (1.0 / D) + EPS)
    normed = (whole * scale * gain).astype(BF16)
    branch = dot(normed, wb_v[...]).astype(BF16)
    gate_in = dot(normed, wg_v[...]).astype(BF16).astype(F32)
    conv_out = old + branch.astype(F32) * taps[3:4]
    gates = jax.nn.sigmoid(dot(conv_out.astype(BF16), bd[...]))
    recur, inject = gates[:, :H], gates[:, H:]
    log_decay = recur * decay
    state = (
        jnp.exp(log_decay) * lru_v[...]
        + jnp.sqrt(1.0 - jnp.exp(2.0 * log_decay)) * inject * conv_out
    )
    state_out[...] = state
    lru_out = (state * jax.nn.gelu(gate_in)).astype(BF16)
    partial = dot(lru_out, wo_v[...]).astype(BF16)
    for k in range(NX):
        part[k] = partial[:, F * k : F * k + F]
    for d in (2, 1, 3):
        remote(part.at[x_idx[d]], mr.at[x], x_sem.at[2], x_sem.at[3], x_dev[d]).start()
    mix = part[x].astype(F32)
    got(mr.at[pl.ds(0, NX - 1)], x_sem.at[3])
    for d in (1, 3, 2):
        mix = mix + mr[x_idx[d]].astype(F32)
    resid = (xg[x].astype(F32) + mix.astype(BF16).astype(F32)).astype(BF16)

    def exchange(way, peers, own, src, dst, s, r):
        for p, dev in peers:
            remote(src.at[p], dst.at[own], s.at[way], r.at[way], dev).start()

    def all_arrived(way, peers, dst, r):
        got(dst.at[pl.ds(0, len(peers))], r.at[way])

    send_a[...] = dot(pick_a[...], resid[:, :H]).astype(BF16).reshape(NG, NZ * CAP, H)
    exchange(0, g_peers, g, send_a, got_a, g_s, g_r)
    send_b[...] = dot(pick_b[...], resid[:, H:]).astype(BF16).reshape(NZ, NG * CAP, H)
    exchange(0, z_peers, z, send_b, got_b, z_s, z_r)
    got_a[g] = send_a[g]
    got_b[z] = send_b[z]
    def to_z(src, dst, s, r):
        for dz in RING8 + (0,):
            i = lax.rem(z + dz, NZ)
            for d in (2, 1, 3, 0):
                if dz or d:
                    remote(src(d, i), dst, s, r, (i * NG + g, x_idx[d])).start()

    def to_g(src, dst, s, r):
        for dy in RING8 + (0,):
            for dc in (1, 0):
                i = lax.rem(y + dy, 8) * 2 + lax.rem(c + dc, 2)
                for d in (2, 1, 3, 0):
                    if dy or dc or d:
                        remote(src(d, i), dst, s, r, (z * NG + i, x_idx[d])).start()

    all_arrived(0, z_peers, got_b, z_r)
    fwd_b[...] = dot(to_gz[...], got_b[...].reshape(ROWS, H)).astype(BF16).reshape(NG, NZ * CAP, H)
    to_g(lambda d, i: fwd_b.at[i], all_b.at[x, g], g_s.at[3], shard_b.at[x])
    all_arrived(0, g_peers, got_a, g_r)
    fwd_a[...] = dot(to_zg[...], got_a[...].reshape(ROWS, H)).astype(BF16).reshape(NZ, NG * CAP, H)
    to_z(lambda d, i: fwd_a.at[i], all_a.at[x, z], z_s.at[3], shard_a.at[x])
    all_a[x, z] = fwd_a[z]
    all_b[x, g] = fwd_b[g]
    left, half_way, right = x_idx[3], x_idx[2], x_idx[1]

    loads["ffng"].wait()
    gain = ffng_v[...].reshape(1, D).astype(F32)
    for k in range(NX):
        gains[k] = gain[:, F * k : F * k + F]
    for name in ("eg", "eu", "ed"):
        loads[name].wait()
    squares = jnp.zeros((ROWS, H), F32)
    for n, k in enumerate((x, left, right, half_way)):
        got(all_a.at[k] if n else all_a.at[k, pl.ds(0, NZ - 1)], shard_a.at[k])
        got(all_b.at[k] if n else all_b.at[k, pl.ds(0, NG - 1)], shard_b.at[k])
        a = all_a[k].reshape(ROWS, H).astype(F32)
        b = dot(to_zg[...], all_b[k].reshape(ROWS, H))
        squares = squares + a * a + b * b
        rows = (jnp.concatenate([a, b], axis=1) * gains[k]).astype(BF16)
        at = pl.ds(pl.multiple_of(k * F, F), F)
        first = dot(rows, eg_v[0, at, :])
        second = dot(rows, eu_v[0, at, :])
        if n == 0:
            acc_g[...] = first
            acc_u[...] = second
        elif n < 3:
            acc_g[...] += first
            acc_u[...] += second
    scale = lax.rsqrt(jnp.sum(squares, axis=1, keepdims=True) * (1.0 / D) + EPS)
    first = (acc_g[...] + first) * scale
    second = (acc_u[...] + second) * scale
    hidden = (first * jax.nn.sigmoid(first) * second).astype(BF16)

    def down(d):
        k = x_idx[d]
        at = pl.ds(pl.multiple_of(k * F, F), F)
        term = dot(hidden, ed_v[0, :, at]).astype(BF16)
        term_a[d] = term[:, :H].reshape(NZ, NG * CAP, H)
        b = dot(to_gz[...], term[:, H:]).astype(BF16)
        term_b[d] = b.reshape(NG, NZ * CAP, H)
        for dy in RING8 + (0,):
            i = lax.rem(z + dy, NZ)
            if dy or d:
                dev = (i * NG + g, k)
                remote(term_a.at[d, i], hop_a.at[x * NZ + z], z_s.at[1], z_r.at[1], dev).start()
            for dc in (1, 0):
                i = lax.rem(y + dy, 8) * 2 + lax.rem(c + dc, 2)
                if dy or dc or d:
                    dev = (z * NG + i, k)
                    remote(term_b.at[d, i], hop_b.at[x * NG + g], g_s.at[1], g_r.at[1], dev).start()

    for d in (2, 1, 3, 0):
        down(d)
    hop_a[x * NZ + z] = term_a[0, z]
    hop_b[x * NG + g] = term_b[0, g]
    got(hop_a.at[pl.ds(0, NX * NZ - 1)], z_r.at[1])
    a = hop_a[...].reshape(NX, ROWS, H).astype(F32)
    a = (a[0] + a[1] + a[2] + a[3]).astype(BF16)
    mid_a[...] = dot(to_gz[...], a).astype(BF16).reshape(NG, NZ * CAP, H)
    exchange(2, g_peers, g, mid_a, back_a, g_s, g_r)
    got(hop_b.at[pl.ds(0, NX * NG - 1)], g_r.at[1])
    b = hop_b[...].reshape(NX, ROWS, H).astype(F32)
    b = (b[0] + b[1] + b[2] + b[3]).astype(BF16)
    mid_b[...] = dot(to_zg[...], b).astype(BF16).reshape(NZ, NG * CAP, H)
    exchange(2, z_peers, z, mid_b, back_b, z_s, z_r)
    back_a[g] = mid_a[g]
    back_b[z] = mid_b[z]
    all_arrived(2, g_peers, back_a, g_r)
    all_arrived(2, z_peers, back_b, z_r)
    for half, comb, back in ((0, comb_a, back_a), (1, comb_b, back_b)):
        rows = back[...].reshape(ROWS, H)
        moe = dot(comb[:, 0:ROWS], rows) + dot(comb[:, ROWS:], rows)
        at = slice(H * half, H * half + H)
        mixed_out[:, at] = (resid[:, at].astype(F32) + moe).astype(BF16)

    sent(xg.at[pl.ds(0, NX - 1)], x_sem.at[0])
    sent(part.at[pl.ds(0, NX - 1)], x_sem.at[2])
    for way in (0, 2):
        sent(send_a.at[pl.ds(0, NG - 1)], g_s.at[way])
        sent(send_b.at[pl.ds(0, NZ - 1)], z_s.at[way])
    for way in (1, 3):
        sent(hop_a.at[pl.ds(0, NX * NZ - 1)], z_s.at[way])
        sent(hop_b.at[pl.ds(0, NX * NG - 1)], g_s.at[way])


def body(
    tokens,
    conv_state,
    lru_state,
    mix_gain,
    ffn_gain,
    w_branch,
    w_gate,
    conv_taps,
    w_recur,
    w_inject,
    lru_lambda,
    w_out,
    expert_gate,
    expert_up,
    expert_down,
    route_ids,
    route_weight,
):
    conv_state = jnp.transpose(conv_state, (1, 0, 2))
    route_ids = jnp.transpose(route_ids)
    route_weight = jnp.transpose(route_weight)
    lru_lambda = lru_lambda.reshape(1, H)
    operands = (
        tokens,
        conv_state,
        lru_state,
        mix_gain,
        ffn_gain,
        w_branch,
        w_gate,
        conv_taps,
        w_recur,
        w_inject,
        lru_lambda,
        w_out,
        expert_gate,
        expert_up,
        expert_down,
        route_ids,
        route_weight,
    )

    operands = tuple(pltpu.with_memory_space_constraint(a, pltpu.HBM) for a in operands)

    def vm(*shape, dtype=BF16):
        return pltpu.VMEM(shape, dtype)

    landing = [vm(NX, S, F)]
    landing += [pltpu.VMEM(a.shape, a.dtype) for a in operands[1:]]
    by_g = (NG, NZ * CAP, H)
    by_z = (NZ, NG * CAP, H)
    scratch = landing + [
        vm(H, 2 * H),
        vm(ROWS, S),
        vm(ROWS, S),
        vm(S, 2 * ROWS),
        vm(S, 2 * ROWS),
        vm(ROWS, ROWS),
        vm(ROWS, ROWS),
        vm(NX, S, F),
        vm(NX, S, F),
        vm(*by_g),
        vm(*by_z),
        vm(*by_g),
        vm(*by_z),
        vm(*by_z),
        vm(*by_g),
        vm(NX, *by_z),
        vm(NX, *by_g),
        vm(NX, 1, F, dtype=F32),
        vm(ROWS, expert_gate.shape[2], dtype=F32),
        vm(ROWS, expert_gate.shape[2], dtype=F32),
        vm(NX, *by_z),
        vm(NX, *by_g),
        vm(NX * NZ, NG * CAP, H),
        vm(NX * NG, NZ * CAP, H),
        vm(*by_g),
        vm(*by_z),
        vm(*by_g),
        vm(*by_z),
    ]
    dma = pltpu.SemaphoreType.DMA
    scratch += [
        dma((17,)),
        dma((4,)),
        dma((4,)),
        dma((4,)),
        dma((4,)),
        dma((4,)),
        dma((NX,)),
        dma((NX,)),
    ]
    return pl.pallas_call(
        kernel,
        out_shape=(
            jax.ShapeDtypeStruct((S, F), BF16),
            jax.ShapeDtypeStruct((S, H), F32),
        ),
        in_specs=[pl.BlockSpec(memory_space=pltpu.HBM)] * len(operands),
        out_specs=(
            pl.BlockSpec(memory_space=pltpu.VMEM),
            pl.BlockSpec(memory_space=pltpu.VMEM),
        ),
        scratch_shapes=scratch,
        compiler_params=pltpu.CompilerParams(
            collective_id=0, has_side_effects=True, vmem_limit_bytes=33554432
        ),
        name="layer",
    )(*operands)


def solution(mesh):
    placed = (
        P("ep", "tp"),
        P("ep", None, "tp"),
        P("ep", "tp"),
        P(),
        P(),
        P(None, "tp"),
        P(None, "tp"),
        P(None, "tp"),
        P("tp", None, None),
        P("tp", None, None),
        P("tp"),
        P("tp", None),
        P("ep", None, "tp"),
        P("ep", None, "tp"),
        P("ep", "tp", None),
        P("ep", None),
        P("ep", None),
    )
    return jax.shard_map(
        body, mesh=mesh, in_specs=placed, out_specs=(P("ep", "tp"), P("ep", "tp")), check_vma=False
    )
```

```python
import functools

import jax
import jax.numpy as jnp
from jax import lax
from jax.experimental import pallas as pl
from jax.experimental.pallas import tpu as pltpu
from jax.sharding import PartitionSpec as P

EPS = 1e-06
LRU_SCALE = 8.0
MESH = pl.DeviceIdType.MESH
F32 = jnp.float32
BF16 = jnp.bfloat16

NX = 4
NZ = 8
NG = 16
S = 64
CAP = 2
F = 256
H = 128
ROWS = NZ * NG * CAP
CH = 1
CR = ROWS // CH
D = NX * F

RING8 = (4, 3, 5, 2, 6, 1, 7)


def remote(src, dst, send, recv, dev):
    return pltpu.make_async_remote_copy(
        src_ref=src, dst_ref=dst, send_sem=send, recv_sem=recv, device_id=dev, device_id_type=MESH
    )


def iota(shape, dim):
    return lax.broadcasted_iota(jnp.int32, shape, dim)


def dot(a, b):
    return jnp.dot(a, b, preferred_element_type=F32)


def swap_matrix(outer, inner):
    row = iota((ROWS, ROWS), 0)
    col = iota((ROWS, ROWS), 1)
    slot = lax.rem(row, CAP)
    mid = lax.rem(lax.div(row, CAP), inner)
    top = lax.div(row, CAP * inner)
    source = mid * (outer * CAP) + top * CAP + slot
    return jnp.where(col == source, 1.0, 0.0).astype(BF16)


def kernel(
    tokens,
    conv_state,
    lru_state,
    mix_gain,
    ffn_gain,
    w_branch,
    w_gate,
    conv_taps,
    w_recur,
    w_inject,
    lru_lambda,
    w_out,
    expert_gate,
    expert_up,
    expert_down,
    ids,
    weights,
    mixed_out,
    state_out,
    xg,
    conv_v,
    lru_v,
    mixg_v,
    ffng_v,
    wb_v,
    wg_v,
    taps_v,
    wr_v,
    wi_v,
    lam_v,
    wo_v,
    eg_v,
    eu_v,
    ed_v,
    ids_v,
    rw_v,
    bd,
    pick_a,
    pick_b,
    comb_a,
    comb_b,
    to_zg,
    to_gz,
    part,
    mr,
    send_a,
    send_b,
    got_a,
    got_b,
    fwd_a,
    fwd_b,
    all_a,
    all_b,
    xn,
    flat_b,
    term_a,
    term_b,
    hop_a,
    hop_b,
    mid_a,
    mid_b,
    back_a,
    back_b,
    in_sem,
    x_sem,
    g_s,
    g_r,
    z_s,
    z_r,
    shard_a,
    shard_b,
):
    x = lax.axis_index("tp")
    e = lax.axis_index("ep")
    z = lax.div(e, NG)
    g = lax.rem(e, NG)
    y = lax.div(g, 2)
    c = lax.rem(g, 2)

    x_dev = [(e, lax.rem(x + d, NX)) for d in range(NX)]
    x_idx = [lax.rem(x + d, NX) for d in range(NX)]
    z_peers = []
    for dz in RING8:
        i = lax.rem(z + dz, NZ)
        z_peers.append((i, (i * NG + g, x)))
    g_peers = []
    for dy in RING8 + (0,):
        for dc in (0, 1):
            if dy or dc:
                i = lax.rem(y + dy, 8) * 2 + lax.rem(c + dc, 2)
                g_peers.append((i, (z * NG + i, x)))

    barrier = pltpu.get_barrier_semaphore()
    for _, dev in z_peers + g_peers:
        pl.semaphore_signal(barrier, inc=1, device_id=dev, device_id_type=MESH)
    for dev in x_dev[1:]:
        pl.semaphore_signal(barrier, inc=1, device_id=dev, device_id_type=MESH)

    loads = {}
    pairs = (
        ("tok", tokens, xg.at[x]),
        ("ids", ids, ids_v),
        ("rw", weights, rw_v),
        ("mixg", mix_gain, mixg_v),
        ("conv", conv_state, conv_v),
        ("taps", conv_taps, taps_v),
        ("wb", w_branch, wb_v),
        ("wg", w_gate, wg_v),
        ("wr", w_recur, wr_v),
        ("wi", w_inject, wi_v),
        ("lam", lru_lambda, lam_v),
        ("lru", lru_state, lru_v),
        ("wo", w_out, wo_v),
        ("ffng", ffn_gain, ffng_v),
        ("eg", expert_gate, eg_v),
        ("eu", expert_up, eu_v),
        ("ed", expert_down, ed_v),
    )
    for i, (name, src, dst) in enumerate(pairs):
        loads[name] = pltpu.make_async_copy(src, dst, in_sem.at[i])
        loads[name].start()

    loads["tok"].wait()
    pl.semaphore_wait(barrier, len(z_peers) + len(g_peers) + NX - 1)

    near = x_dev[1]

    def got(dst, sem):
        remote(dst, dst, sem, sem, near).wait_recv()

    def sent(src, sem):
        remote(src, src, sem, sem, near).wait_send()

    for d in (2, 1, 3):
        remote(xg.at[x], xg.at[x], x_sem.at[0], x_sem.at[1], x_dev[d]).start()

    loads["ids"].wait()
    loads["rw"].wait()
    for pick, comb, outer, inner in ((pick_a, comb_a, NG, NZ), (pick_b, comb_b, NZ, NG)):
        row = iota((ROWS, S), 0)
        slot = lax.rem(row, CAP).astype(F32)
        first = lax.rem(lax.div(row, CAP), inner)
        second = lax.div(row, CAP * inner)
        expert = first * NG + second if outer == NG else second * NG + first
        hit0 = jnp.where(ids_v[0:1, :] == expert, 1.0, 0.0)
        hit1 = jnp.where(ids_v[1:2, :] == expert, 1.0, 0.0)
        hit = hit0 + hit1
        earlier = jnp.where(iota((S, S), 0) < iota((S, S), 1), 1.0, 0.0).astype(BF16)
        before = dot(hit.astype(BF16), earlier)
        chosen = jnp.where(before == slot, hit, 0.0)
        pick[...] = chosen.astype(BF16)
        weight = jnp.where(before == slot, hit0 * rw_v[0:1, :] + hit1 * rw_v[1:2, :], 0.0)
        weight = jnp.transpose(weight)
        high = weight.astype(BF16)
        comb[:, 0:ROWS] = high
        comb[:, ROWS:] = (weight - high.astype(F32)).astype(BF16)
    to_zg[...] = swap_matrix(NZ, NG)
    to_gz[...] = swap_matrix(NG, NZ)

    loads["wr"].wait()
    loads["wi"].wait()
    bd[...] = jnp.zeros_like(bd)
    for h in range(2):
        lo, hi = 64 * h, 64 * h + 64
        for k, w in enumerate((wr_v, wi_v)):
            bd[lo:hi, H * k + lo : H * k + hi] = w[h]
    loads["conv"].wait()
    loads["taps"].wait()
    taps = taps_v[...].astype(F32)
    old = (
        conv_v[0].astype(F32) * taps[0:1]
        + conv_v[1].astype(F32) * taps[1:2]
        + conv_v[2].astype(F32) * taps[2:3]
    )
    loads["lam"].wait()
    decay = -LRU_SCALE * jax.nn.softplus(-lam_v[...])
    loads["lru"].wait()
    loads["mixg"].wait()
    gain = mixg_v[...].reshape(1, D).astype(F32)
    for name in ("wb", "wg", "wo"):
        loads[name].wait()

    got(xg.at[pl.ds(0, NX - 1)], x_sem.at[1])
    whole = jnp.concatenate([xg[k].astype(F32) for k in range(NX)], axis=1)
    scale = lax.rsqrt(jnp.sum(whole * whole, axis=1, keepdims=True) * (1.0 / D) + EPS)
    normed = (whole * scale * gain).astype(BF16)
    branch = dot(normed, wb_v[...]).astype(BF16)
    gate_in = dot(normed, wg_v[...]).astype(BF16).astype(F32)
    conv_out = old + branch.astype(F32) * taps[3:4]
    gates = jax.nn.sigmoid(dot(conv_out.astype(BF16), bd[...]))
    recur, inject = gates[:, :H], gates[:, H:]
    log_decay = recur * decay
    state = (
        jnp.exp(log_decay) * lru_v[...]
        + jnp.sqrt(1.0 - jnp.exp(2.0 * log_decay)) * inject * conv_out
    )
    state_out[...] = state
    lru_out = (state * jax.nn.gelu(gate_in)).astype(BF16)
    partial = dot(lru_out, wo_v[...]).astype(BF16)
    for k in range(NX):
        part[k] = partial[:, F * k : F * k + F]
    for d in (2, 1, 3):
        remote(part.at[x_idx[d]], mr.at[x], x_sem.at[2], x_sem.at[3], x_dev[d]).start()
    mix = part[x].astype(F32)
    got(mr.at[pl.ds(0, NX - 1)], x_sem.at[3])
    for d in (1, 3, 2):
        mix = mix + mr[x_idx[d]].astype(F32)
    resid = (xg[x].astype(F32) + mix.astype(BF16).astype(F32)).astype(BF16)

    def exchange(way, peers, own, src, dst, s, r):
        for p, dev in peers:
            remote(src.at[p], dst.at[own], s.at[way], r.at[way], dev).start()

    def all_arrived(way, peers, dst, r):
        got(dst.at[pl.ds(0, len(peers))], r.at[way])

    send_a[...] = dot(pick_a[...], resid[:, :H]).astype(BF16).reshape(NG, NZ * CAP, H)
    exchange(0, g_peers, g, send_a, got_a, g_s, g_r)
    send_b[...] = dot(pick_b[...], resid[:, H:]).astype(BF16).reshape(NZ, NG * CAP, H)
    exchange(0, z_peers, z, send_b, got_b, z_s, z_r)
    got_a[g] = send_a[g]
    got_b[z] = send_b[z]
    def to_z(src, dst, s, r):
        for d in (2, 1, 3, 0):
            for dz in RING8 + (0,):
                i = lax.rem(z + dz, NZ)
                if dz or d:
                    remote(src(d, i), dst, s, r, (i * NG + g, x_idx[d])).start()

    def to_g(src, dst, s, r):
        for d in (2, 1, 3, 0):
            for dy, dc in ((dy, dc) for dy in RING8 + (0,) for dc in (1, 0)):
                i = lax.rem(y + dy, 8) * 2 + lax.rem(c + dc, 2)
                if dy or dc or d:
                    remote(src(d, i), dst, s, r, (z * NG + i, x_idx[d])).start()

    all_arrived(0, z_peers, got_b, z_r)
    fwd_b[...] = dot(to_gz[...], got_b[...].reshape(ROWS, H)).astype(BF16).reshape(NG, NZ * CAP, H)
    to_g(lambda d, i: fwd_b.at[i], all_b.at[x, g], g_s.at[3], shard_b.at[x])
    all_arrived(0, g_peers, got_a, g_r)
    fwd_a[...] = dot(to_zg[...], got_a[...].reshape(ROWS, H)).astype(BF16).reshape(NZ, NG * CAP, H)
    to_z(lambda d, i: fwd_a.at[i], all_a.at[x, z], z_s.at[3], shard_a.at[x])
    all_a[x, z] = fwd_a[z]
    all_b[x, g] = fwd_b[g]

    loads["ffng"].wait()
    gain = ffng_v[...].reshape(1, D).astype(F32)
    for name in ("eg", "eu", "ed"):
        loads[name].wait()
    got(all_a.at[x, pl.ds(0, NZ - 1)], shard_a.at[x])
    got(all_b.at[x, pl.ds(0, NG - 1)], shard_b.at[x])
    for k in x_idx[1:]:
        got(all_a.at[k], shard_a.at[k])
        got(all_b.at[k], shard_b.at[k])
    full_b = jnp.concatenate([all_b[k].reshape(ROWS, H) for k in range(NX)], axis=1)
    full_b = dot(to_zg[...], full_b)
    pieces = []
    for k in range(NX):
        pieces.append(all_a[k].reshape(ROWS, H).astype(F32))
        pieces.append(full_b[:, H * k : H * k + H])
    rows = jnp.concatenate(pieces, axis=1)
    scale = lax.rsqrt(jnp.sum(rows * rows, axis=1, keepdims=True) * (1.0 / D) + EPS)
    xn[...] = (rows * scale * gain).astype(BF16)
    for j in range(CH):
        at = slice(CR * j, CR * j + CR)
        rows = xn[at, :]
        first = dot(rows, eg_v[0])
        second = dot(rows, eu_v[0])
        hidden = (first * jax.nn.sigmoid(first) * second).astype(BF16)
        term = dot(hidden, ed_v[0]).astype(BF16)
        blocks = slice(NZ // CH * j, NZ // CH * (j + 1))
        for k in range(NX):
            term_a[k, blocks] = term[:, F * k : F * k + H].reshape(NZ // CH, NG * CAP, H)
            flat_b[at, H * k : H * k + H] = term[:, F * k + H : F * k + F]

    for d in (2, 1, 3, 0):
        for dz in RING8 + (0,):
            i = lax.rem(z + dz, NZ)
            if dz or d:
                src, dev = term_a.at[x_idx[d], i], (i * NG + g, x_idx[d])
                remote(src, hop_a.at[x * NZ + z], z_s.at[1], z_r.at[1], dev).start()
    swapped = dot(to_gz[...], flat_b[...]).astype(BF16)
    for k in range(NX):
        term_b[k] = swapped[:, H * k : H * k + H].reshape(NG, NZ * CAP, H)
    for d in (2, 1, 3, 0):
        for dy, dc in ((dy, dc) for dy in RING8 + (0,) for dc in (1, 0)):
            i = lax.rem(y + dy, 8) * 2 + lax.rem(c + dc, 2)
            if dy or dc or d:
                src, dev = term_b.at[x_idx[d], i], (z * NG + i, x_idx[d])
                remote(src, hop_b.at[x * NG + g], g_s.at[1], g_r.at[1], dev).start()
    hop_a[x * NZ + z] = term_a[x, z]
    hop_b[x * NG + g] = term_b[x, g]
    got(hop_a.at[pl.ds(0, NX * NZ - 1)], z_r.at[1])
    a = hop_a[...].reshape(NX, ROWS, H).astype(F32)
    a = (a[0] + a[1] + a[2] + a[3]).astype(BF16)
    mid_a[...] = dot(to_gz[...], a).astype(BF16).reshape(NG, NZ * CAP, H)
    exchange(2, g_peers, g, mid_a, back_a, g_s, g_r)
    got(hop_b.at[pl.ds(0, NX * NG - 1)], g_r.at[1])
    b = hop_b[...].reshape(NX, ROWS, H).astype(F32)
    b = (b[0] + b[1] + b[2] + b[3]).astype(BF16)
    mid_b[...] = dot(to_zg[...], b).astype(BF16).reshape(NZ, NG * CAP, H)
    exchange(2, z_peers, z, mid_b, back_b, z_s, z_r)
    back_a[g] = mid_a[g]
    back_b[z] = mid_b[z]
    all_arrived(2, g_peers, back_a, g_r)
    all_arrived(2, z_peers, back_b, z_r)
    for half, comb, back in ((0, comb_a, back_a), (1, comb_b, back_b)):
        rows = back[...].reshape(ROWS, H)
        moe = dot(comb[:, 0:ROWS], rows) + dot(comb[:, ROWS:], rows)
        at = slice(H * half, H * half + H)
        mixed_out[:, at] = (resid[:, at].astype(F32) + moe).astype(BF16)

    sent(xg.at[pl.ds(0, NX - 1)], x_sem.at[0])
    sent(part.at[pl.ds(0, NX - 1)], x_sem.at[2])
    for way in (0, 2):
        sent(send_a.at[pl.ds(0, NG - 1)], g_s.at[way])
        sent(send_b.at[pl.ds(0, NZ - 1)], z_s.at[way])
    for way in (1, 3):
        sent(hop_a.at[pl.ds(0, NX * NZ - 1)], z_s.at[way])
        sent(hop_b.at[pl.ds(0, NX * NG - 1)], g_s.at[way])


def body(
    tokens,
    conv_state,
    lru_state,
    mix_gain,
    ffn_gain,
    w_branch,
    w_gate,
    conv_taps,
    w_recur,
    w_inject,
    lru_lambda,
    w_out,
    expert_gate,
    expert_up,
    expert_down,
    route_ids,
    route_weight,
):
    conv_state = jnp.transpose(conv_state, (1, 0, 2))
    route_ids = jnp.transpose(route_ids)
    route_weight = jnp.transpose(route_weight)
    lru_lambda = lru_lambda.reshape(1, H)
    operands = (
        tokens,
        conv_state,
        lru_state,
        mix_gain,
        ffn_gain,
        w_branch,
        w_gate,
        conv_taps,
        w_recur,
        w_inject,
        lru_lambda,
        w_out,
        expert_gate,
        expert_up,
        expert_down,
        route_ids,
        route_weight,
    )

    operands = tuple(pltpu.with_memory_space_constraint(a, pltpu.HBM) for a in operands)

    def vm(*shape, dtype=BF16):
        return pltpu.VMEM(shape, dtype)

    landing = [vm(NX, S, F)]
    landing += [pltpu.VMEM(a.shape, a.dtype) for a in operands[1:]]
    by_g = (NG, NZ * CAP, H)
    by_z = (NZ, NG * CAP, H)
    scratch = landing + [
        vm(H, 2 * H),
        vm(ROWS, S),
        vm(ROWS, S),
        vm(S, 2 * ROWS),
        vm(S, 2 * ROWS),
        vm(ROWS, ROWS),
        vm(ROWS, ROWS),
        vm(NX, S, F),
        vm(NX, S, F),
        vm(*by_g),
        vm(*by_z),
        vm(*by_g),
        vm(*by_z),
        vm(*by_z),
        vm(*by_g),
        vm(NX, *by_z),
        vm(NX, *by_g),
        vm(ROWS, D),
        vm(ROWS, NX * H),
        vm(NX, *by_z),
        vm(NX, *by_g),
        vm(NX * NZ, NG * CAP, H),
        vm(NX * NG, NZ * CAP, H),
        vm(*by_g),
        vm(*by_z),
        vm(*by_g),
        vm(*by_z),
    ]
    dma = pltpu.SemaphoreType.DMA
    scratch += [
        dma((17,)),
        dma((4,)),
        dma((4,)),
        dma((4,)),
        dma((4,)),
        dma((4,)),
        dma((NX,)),
        dma((NX,)),
    ]
    return pl.pallas_call(
        kernel,
        out_shape=(
            jax.ShapeDtypeStruct((S, F), BF16),
            jax.ShapeDtypeStruct((S, H), F32),
        ),
        in_specs=[pl.BlockSpec(memory_space=pltpu.HBM)] * len(operands),
        out_specs=(
            pl.BlockSpec(memory_space=pltpu.VMEM),
            pl.BlockSpec(memory_space=pltpu.VMEM),
        ),
        scratch_shapes=scratch,
        compiler_params=pltpu.CompilerParams(
            collective_id=0, has_side_effects=True, vmem_limit_bytes=33554432
        ),
        name="layer",
    )(*operands)


def solution(mesh):
    placed = (
        P("ep", "tp"),
        P("ep", None, "tp"),
        P("ep", "tp"),
        P(),
        P(),
        P(None, "tp"),
        P(None, "tp"),
        P(None, "tp"),
        P("tp", None, None),
        P("tp", None, None),
        P("tp"),
        P("tp", None),
        P("ep", None, "tp"),
        P("ep", None, "tp"),
        P("ep", "tp", None),
        P("ep", None),
        P("ep", None),
    )
    return jax.shard_map(
        body, mesh=mesh, in_specs=placed, out_specs=(P("ep", "tp"), P("ep", "tp")), check_vma=False
    )
```
